32 devices in a mesh: sp: 4 (over z), fs: 4 (over y, x), tp: 2 (over core).
Axes of the slice: x: 2, y: 2, z: 4, core: 2. Of those that a mesh axis runs over, the one named last changes fastest.
Arguments:
- tokens: bfloat16 [4, 2048, 2048], P('fs', ('sp', 'tp')), may hold values from -6 to 6
- norm_gain: float32 [2048], replicated, may hold values from 0.1 to 1.9
- query_weight: bfloat16 [2048, 1024], P('sp', 'tp'), may hold values from -20 to 20
- key_matrix: bfloat16 [2048, 256], P('sp', 'tp'), may hold values from -0.125 to 0.125
- value_matrix: bfloat16 [2048, 256], P('sp', 'tp'), may hold values from -0.125 to 0.125
- pool_in_weight: bfloat16 [2048, 1024], P('sp', 'tp'), may hold values from -0.125 to 0.125
- head_sink_logit: float32 [16], replicated, may hold values from 2 to 6
- pool_mix: bfloat16 [4, 256, 256], replicated, may hold values from -0.375 to 0.375
- pool_gain: float32 [1024], replicated, may hold values from 0.1 to 1.9
- attn_out_weight: bfloat16 [1024, 2048], P('tp', 'sp'), may hold values from -1 to 1
- pool_out_weight: bfloat16 [1024, 2048], P('tp', 'sp'), may hold values from -0.125 to 0.125
Outputs:
- mixed: bfloat16 [4, 2048, 2048], P('fs', ('sp', 'tp'))
- row_log_weight_sum: float32 [4, 16, 2048], P('fs', 'tp', 'sp')
The draws below stay inside these ranges and needn't reach their ends.
All inputs are finite; a program needn't handle non-finite values.
Results may differ from the reference program's by a relative error of at most 0.0095.
The reference program's roundings to bfloat16 on the way count: a program that leaves them out, or rounds other values in their place, can miss the bound.
Values may be sent and summed in bfloat16 or wider, within the bound.
No kernel may reach another device: no remote copies, remote signals or barrier semaphores. Data moves between devices by JAX's collectives and lax.ppermute only.
A program may use at most 64 MiB of HBM per device.

```python
import jax
import jax.numpy as jnp
from jax import lax

MODEL_WIDTH = 2048
HEAD_SIZE = 64
QUERY_HEADS = 16
KEY_VALUE_HEADS = 4
WINDOW = 128
POOL_GROUPS = 4
POOL_CH = 256
LEN = 2048
SEQS = 4


def draw_query_weight(key, part):
    base = jax.random.normal(jax.random.fold_in(key, 11), (MODEL_WIDTH, QUERY_HEADS * HEAD_SIZE), jnp.float32)
    base = jnp.clip(base, -6.0, 6.0) * MODEL_WIDTH ** (-0.5)
    return jnp.clip(base, -20.0, 20.0).astype(jnp.bfloat16)


def levels(rng, shape, shards, least, high):
    def one(axis_at, parts):
        heights = jax.random.uniform(jax.random.fold_in(jax.random.fold_in(rng, 6), axis_at), (parts,), jnp.float32, least / len(shards), high / len(shards))
        return jnp.repeat(jnp.exp(heights), shape[axis_at] // parts).reshape((-1,) + (1,) * (len(shape) - axis_at - 1))

    level = one(*shards[0])
    for cut in shards[1:]:
        level = level * one(*cut)
    return level


def bell_draw(rng, extent, deviation, reach, cuts=(), kind=jnp.bfloat16):
    values = deviation * jax.random.normal(rng, extent, jnp.float32)
    if cuts:
        values = values * levels(rng, extent, cuts, -0.22, 0.18)
    return jnp.clip(values, -reach, reach).astype(kind)


def setup_inputs(seed: int = 0) -> dict:
    seeds = jax.random.split(jax.random.key(seed), 12)
    return {
        "tokens": bell_draw(seeds[0], (SEQS, LEN, MODEL_WIDTH), 1.0, 6.0, ((0, 4), (1, 8))),
        "norm_gain": jnp.clip(1.0 + 0.18 * jax.random.normal(seeds[1], (MODEL_WIDTH,), jnp.float32), 0.1, 1.9),
        "query_weight": draw_query_weight(jax.random.fold_in(seeds[11], 71), 0),
        "key_matrix": bell_draw(seeds[3], (MODEL_WIDTH, KEY_VALUE_HEADS * HEAD_SIZE), MODEL_WIDTH ** -0.5, 0.125, ((0, 4), (1, 2))),
        "value_matrix": bell_draw(seeds[4], (MODEL_WIDTH, KEY_VALUE_HEADS * HEAD_SIZE), MODEL_WIDTH ** -0.5, 0.125, ((0, 4), (1, 2))),
        "pool_in_weight": bell_draw(seeds[5], (MODEL_WIDTH, POOL_GROUPS * POOL_CH), MODEL_WIDTH ** -0.5, 0.125, ((0, 4), (1, 2))),
        "head_sink_logit": jnp.clip(jax.random.uniform(seeds[6], (QUERY_HEADS,), jnp.float32, 2.0, 6.0), 2.0, 6.0),
        "pool_mix": bell_draw(seeds[7], (POOL_GROUPS, POOL_CH, POOL_CH), POOL_CH ** -0.5, 0.375),
        "pool_gain": jnp.clip(1.0 + 0.18 * jax.random.normal(seeds[8], (POOL_GROUPS * POOL_CH,), jnp.float32), 0.1, 1.9),
        "attn_out_weight": bell_draw(seeds[9], (QUERY_HEADS * HEAD_SIZE, MODEL_WIDTH), (QUERY_HEADS * HEAD_SIZE // 32) ** -0.5, 1.0, ((0, 2), (1, 4))),
        "pool_out_weight": bell_draw(seeds[10], (POOL_GROUPS * POOL_CH, MODEL_WIDTH), (QUERY_HEADS * HEAD_SIZE + POOL_GROUPS * POOL_CH) ** -0.5, 0.125, ((0, 2), (1, 4))),
    }


EPSILON = 1e-06
POOL_SPANS = (2, 4, 8, 16)

def windowed_attend(query_rows, key_rows, value_rows, sinks, kv_heads, group):
    rows = query_rows.shape[0]
    blocks = rows // WINDOW
    width = key_rows.shape[1]
    ext_keys = jnp.concatenate([jnp.zeros((WINDOW, width), key_rows.dtype), key_rows], 0)
    ext_values = jnp.concatenate([jnp.zeros((WINDOW, width), value_rows.dtype), value_rows], 0)

    def banded(table):
        return jnp.concatenate([table[:rows].reshape(blocks, WINDOW, width), table[WINDOW:].reshape(blocks, WINDOW, width)], axis=1)
    band_keys = banded(ext_keys).reshape(blocks, 2 * WINDOW, kv_heads, HEAD_SIZE).astype(jnp.float32)
    band_values = banded(ext_values).reshape(blocks, 2 * WINDOW, kv_heads, HEAD_SIZE).astype(jnp.float32)
    query_blocks = query_rows.reshape(blocks, WINDOW, kv_heads, group, HEAD_SIZE).astype(jnp.float32)
    scores = jnp.einsum('bqkgd,bskd->bkgqs', query_blocks, band_keys) * HEAD_SIZE ** (-0.5)
    query_pos = jnp.arange(rows).reshape(blocks, WINDOW, 1)
    key_pos = jnp.arange(blocks).reshape(blocks, 1, 1) * WINDOW - WINDOW + jnp.arange(2 * WINDOW).reshape(1, 1, 2 * WINDOW)
    offset = query_pos - key_pos
    allowed = (offset >= 0) & (offset < WINDOW) & (key_pos >= 0)
    scores = jnp.where(allowed[:, None, None], scores, -jnp.inf)
    sink_grid = sinks.astype(jnp.float32).reshape(1, kv_heads, group, 1, 1)
    top = jnp.maximum(lax.optimization_barrier(jnp.max(scores, axis=-1, keepdims=True)), sink_grid)
    weights = jnp.exp(scores - top)
    total = lax.optimization_barrier(jnp.sum(weights, axis=-1, keepdims=True)) + jnp.exp(sink_grid - top)
    probs = (weights / total).astype(jnp.bfloat16).astype(jnp.float32)
    mixed = jnp.einsum('bkgqs,bskd->bqkgd', probs, band_values).astype(jnp.bfloat16)
    row_log_weight_sum = (top + jnp.log(total))[..., 0]
    return (mixed.reshape(rows, kv_heads * group * HEAD_SIZE), row_log_weight_sum.transpose(1, 2, 0, 3).reshape(kv_heads * group, rows))

def pool_branch(pool_input, pool_mix, pool_gain):
    rows = pool_input.shape[0]
    pool_reach = max(POOL_SPANS)
    padded = jnp.concatenate([jnp.zeros((pool_reach, pool_input.shape[1]), jnp.float32), pool_input.astype(jnp.float32)], 0)
    position = jnp.arange(rows).reshape(rows, 1)
    pieces = []
    for index, span in enumerate(POOL_SPANS):
        columns = padded[:, index * POOL_CH:(index + 1) * POOL_CH]
        trailing = jnp.zeros((rows, POOL_CH), jnp.float32)
        for lag in range(span):
            trailing = trailing + columns[pool_reach - lag:pool_reach - lag + rows]
        count = jnp.minimum(position + 1, span).astype(jnp.float32)
        pieces.append(trailing / count - columns[pool_reach:])
    centred = jnp.concatenate(pieces, axis=1).astype(jnp.bfloat16)
    grouped = centred.reshape(rows, POOL_GROUPS, POOL_CH).astype(jnp.float32)
    product = jnp.einsum('rgc,gcd->rgd', grouped, pool_mix.astype(jnp.float32)).reshape(rows, POOL_GROUPS * POOL_CH)
    return (product * pool_gain).astype(jnp.bfloat16)

def reference(tokens, norm_gain, query_weight, key_matrix, value_matrix, pool_in_weight, head_sink_logit, pool_mix, pool_gain, attn_out_weight, pool_out_weight):

    def one_sequence(sequence):
        values_f = sequence.astype(jnp.float32)
        scale = lax.rsqrt(lax.optimization_barrier(jnp.mean(values_f * values_f, axis=-1, keepdims=True)) + EPSILON)
        normed = (values_f * scale * norm_gain).astype(jnp.bfloat16)
        query_rows = jnp.dot(normed, query_weight, preferred_element_type=jnp.float32).astype(jnp.bfloat16)
        key_rows = jnp.dot(normed, key_matrix, preferred_element_type=jnp.float32).astype(jnp.bfloat16)
        value_rows = jnp.dot(normed, value_matrix, preferred_element_type=jnp.float32).astype(jnp.bfloat16)
        pool_input = jnp.dot(normed, pool_in_weight, preferred_element_type=jnp.float32).astype(jnp.bfloat16)
        attention_mixer, row_log_weight_sum = windowed_attend(query_rows, key_rows, value_rows, head_sink_logit, KEY_VALUE_HEADS, QUERY_HEADS // KEY_VALUE_HEADS)
        pool_out = pool_branch(pool_input, pool_mix, pool_gain)
        result = jnp.dot(attention_mixer, attn_out_weight, preferred_element_type=jnp.float32) + jnp.dot(pool_out, pool_out_weight, preferred_element_type=jnp.float32)
        return (result.astype(jnp.bfloat16), row_log_weight_sum)
    mixed, row_log_weight_sum = lax.map(one_sequence, tokens)
    return (mixed, row_log_weight_sum)
```

```python
import jax
import jax.numpy as jnp
from jax import lax
from jax.sharding import PartitionSpec as P

HEAD_SIZE = 64
WINDOW = 128
POOL_CH = 256


EPSILON = 1e-06
POOL_SPANS = (2, 4, 8, 16)


def passed_along(shard, axis, by):
    size = lax.axis_size(axis)
    pairs = [(i, i + by) for i in range(size) if 0 <= i + by < size]
    return lax.ppermute(shard, axis, pairs)


def windowed_attend(
    query_rows, key_rows, value_rows, key_tail, value_tail, sinks, kv_heads, group, first_pos
):
    rows = query_rows.shape[0]
    blocks = rows // WINDOW
    width = key_rows.shape[1]
    ext_keys = jnp.concatenate([key_tail, key_rows], 0)
    ext_values = jnp.concatenate([value_tail, value_rows], 0)

    def banded(table):
        return jnp.concatenate(
            [
                table[:rows].reshape(blocks, WINDOW, width),
                table[WINDOW:].reshape(blocks, WINDOW, width),
            ],
            axis=1,
        )

    band_keys = banded(ext_keys).reshape(blocks, 2 * WINDOW, kv_heads, HEAD_SIZE)
    band_values = banded(ext_values).reshape(blocks, 2 * WINDOW, kv_heads, HEAD_SIZE)
    query_blocks = query_rows.reshape(blocks, WINDOW, kv_heads, group, HEAD_SIZE)
    scores = jnp.einsum(
        "bqkgd,bskd->bkgqs", query_blocks, band_keys, preferred_element_type=jnp.float32
    ) * HEAD_SIZE ** (-0.5)
    query_pos = first_pos + jnp.arange(rows).reshape(blocks, WINDOW, 1)
    key_pos = (
        first_pos
        - WINDOW
        + jnp.arange(blocks).reshape(blocks, 1, 1) * WINDOW
        + jnp.arange(2 * WINDOW).reshape(1, 1, 2 * WINDOW)
    )
    offset = query_pos - key_pos
    allowed = (offset >= 0) & (offset < WINDOW) & (key_pos >= 0)
    scores = jnp.where(allowed[:, None, None], scores, -jnp.inf)
    sink_grid = sinks.reshape(1, kv_heads, group, 1, 1)
    top = jnp.maximum(jnp.max(scores, axis=-1, keepdims=True), sink_grid)
    weights = jnp.exp(scores - top)
    total = jnp.sum(weights, axis=-1, keepdims=True) + jnp.exp(sink_grid - top)
    probs = (weights / total).astype(jnp.bfloat16)
    mixed = jnp.einsum(
        "bkgqs,bskd->bqkgd", probs, band_values, preferred_element_type=jnp.float32
    ).astype(jnp.bfloat16)
    row_log_weight_sum = (top + jnp.log(total))[..., 0]
    return (
        mixed.reshape(rows, kv_heads * group * HEAD_SIZE),
        row_log_weight_sum.transpose(1, 2, 0, 3).reshape(kv_heads * group, rows),
    )


def pool_branch(pool_rows, pool_tail, mixing, scales, group_start, first_pos):
    rows = pool_rows.shape[0]
    columns = pool_rows.shape[1]
    pool_reach = max(POOL_SPANS)
    extended = jnp.concatenate([pool_tail, pool_rows], 0).astype(jnp.float32)
    group_index = group_start + jnp.arange(columns) // POOL_CH
    span_table = jnp.array(POOL_SPANS, jnp.int32)
    matches = group_index[:, None] == jnp.arange(len(POOL_SPANS))[None, :]
    span_of_col = jnp.sum(jnp.where(matches, span_table[None, :], 0), axis=1)
    trailing = jnp.zeros((rows, columns), jnp.float32)
    for lag in range(pool_reach):
        trailing = trailing + jnp.where(
            lag < span_of_col[None, :], extended[pool_reach - lag : pool_reach - lag + rows], 0.0
        )
    position = first_pos + jnp.arange(rows)
    count = jnp.minimum(position[:, None] + 1, span_of_col[None, :]).astype(jnp.float32)
    centred = (trailing / count - extended[pool_reach:]).astype(jnp.bfloat16)
    grouped = centred.reshape(rows, columns // POOL_CH, POOL_CH)
    product = jnp.einsum(
        "rgc,gcd->rgd", grouped, mixing, preferred_element_type=jnp.float32
    ).reshape(rows, columns)
    return (product * scales).astype(jnp.bfloat16)


def swapped(axis, bit):
    return [(i, i ^ bit) for i in range(lax.axis_size(axis))]


def gathered_shards(shard, axis):
    size = lax.axis_size("sp")
    members = lax.axis_size("fs")
    here = lax.axis_index("sp")
    if members != 4 or size > 8:
        return [(0, [(0, lax.all_gather(shard, "sp", axis=axis, tiled=True))])]
    fs_index = lax.axis_index("fs")
    quarter = shard.shape[0] // members
    mine = lax.dynamic_slice_in_dim(shard, fs_index * quarter, quarter, 0)
    gathered = [(here, [(0, shard)])]
    shifts = sorted(range(1, size), key=lambda d: (min(d, size - d), d))
    along = [
        lax.ppermute(mine, "sp", [(i, (i + d) % size) for i in range(size)]) for d in shifts
    ]
    for batch in (slice(0, 2), slice(2, None)):
        picked = along[batch]
        if not picked:
            continue
        own = jnp.concatenate(picked, 0)
        near = lax.ppermute(own, "fs", swapped("fs", 1))
        far = lax.ppermute(own, "fs", swapped("fs", 2))
        half = own.shape[1] // 2 // 128 * 128
        corner = jnp.concatenate(
            [
                lax.ppermute(near[:, :half], "fs", swapped("fs", 2)),
                lax.ppermute(far[:, half:], "fs", swapped("fs", 1)),
            ],
            axis=1,
        )
        for k, d in enumerate(shifts[batch]):
            cut = slice(k * quarter, (k + 1) * quarter)
            gathered.append(
                (
                    (here - d) % size,
                    [
                        (fs_index, own[cut]),
                        (fs_index ^ 1, near[cut]),
                        (fs_index ^ 2, far[cut]),
                        (fs_index ^ 3, corner[cut]),
                    ],
                )
            )
    return gathered


def local(
    tokens,
    norm_gain,
    query_weight,
    key_matrix,
    value_matrix,
    pool_in_weight,
    head_sink_logit,
    pool_mix,
    pool_gain,
    attn_out_weight,
    pool_out_weight,
):
    tp_index = lax.axis_index("tp")
    sp_index = lax.axis_index("sp")
    q_cols = query_weight.shape[1]
    kv_cols = key_matrix.shape[1]
    pool_cols = pool_in_weight.shape[1]
    q_heads = q_cols // HEAD_SIZE
    kv_heads = kv_cols // HEAD_SIZE
    groups_dev = pool_cols // POOL_CH
    in_weight = jnp.concatenate([query_weight, key_matrix, value_matrix, pool_in_weight], axis=1)
    out_weight = jnp.concatenate([attn_out_weight, pool_out_weight], axis=0)
    wide = q_cols + 2 * kv_cols + pool_cols
    in_gathered = gathered_shards(in_weight, 0)
    out_gathered = gathered_shards(out_weight, 1)
    own = tokens[0].astype(jnp.float32)
    scale = lax.rsqrt(jnp.mean(own * own, axis=-1, keepdims=True) + EPSILON)
    normed_own = (own * scale * norm_gain).astype(jnp.bfloat16)
    normed_peer = lax.ppermute(normed_own, "tp", swapped("tp", 1))
    half_rows = normed_own.shape[0]
    rows = 2 * half_rows
    first = tp_index == 0
    normed = jnp.concatenate(
        [jnp.where(first, normed_own, normed_peer), jnp.where(first, normed_peer, normed_own)], 0
    )
    shard_rows = in_weight.shape[0]
    total = jnp.zeros((rows, wide), jnp.float32)
    for source, quarters in in_gathered:
        if len(quarters) == 1:
            left = lax.dynamic_slice_in_dim(
                normed, source * shard_rows, quarters[0][1].shape[0], 1
            )
        else:
            left = jnp.concatenate(
                [
                    lax.dynamic_slice_in_dim(
                        normed, source * shard_rows + member * part.shape[0], part.shape[0], 1
                    )
                    for member, part in quarters
                ],
                axis=1,
            )
        right = jnp.concatenate([part for _, part in quarters], axis=0)
        total = total + jnp.dot(left, right, preferred_element_type=jnp.float32)
    projected = total.astype(jnp.bfloat16)
    first_pos = sp_index * rows
    query_rows = projected[:, :q_cols]
    key_rows = projected[:, q_cols : q_cols + kv_cols]
    value_rows = projected[:, q_cols + kv_cols : q_cols + 2 * kv_cols]
    pool_rows = projected[:, q_cols + 2 * kv_cols :]
    pool_reach = max(POOL_SPANS)
    sinks = lax.dynamic_slice_in_dim(head_sink_logit, tp_index * q_heads, q_heads, 0)
    mixing = lax.dynamic_slice_in_dim(pool_mix, tp_index * groups_dev, groups_dev, 0)
    scales = lax.dynamic_slice_in_dim(pool_gain, tp_index * pool_cols, pool_cols, 0)
    kv_tail = projected[rows - WINDOW :, q_cols : q_cols + 2 * kv_cols]
    packed = pool_rows[rows - pool_reach :].reshape(-1, 2 * kv_cols)
    tail = passed_along(jnp.concatenate([kv_tail, packed], 0), "sp", 1)
    key_tail = tail[:WINDOW, :kv_cols]
    value_tail = tail[:WINDOW, kv_cols:]
    pool_tail = tail[WINDOW:].reshape(pool_reach, pool_cols)
    attn_part, log_part = windowed_attend(
        query_rows,
        key_rows,
        value_rows,
        key_tail,
        value_tail,
        sinks,
        kv_heads,
        q_heads // kv_heads,
        first_pos,
    )
    pool_part = pool_branch(pool_rows, pool_tail, mixing, scales, tp_index * groups_dev, first_pos)
    mixers = jnp.concatenate([attn_part, pool_part], axis=1)
    shard_cols = out_weight.shape[1]
    sides = [
        lax.dynamic_slice_in_dim(mixers, side * half_rows, half_rows, 0)
        for side in (1 - tp_index, tp_index)
    ]
    sums = []
    for side in sides:
        result = jnp.zeros((half_rows, shard_cols * lax.axis_size("sp")), jnp.float32)
        for source, quarters in out_gathered:
            if len(quarters) == 1:
                left = side
            else:
                left = jnp.concatenate(
                    [
                        lax.dynamic_slice_in_dim(side, member * part.shape[0], part.shape[0], 1)
                        for member, part in quarters
                    ],
                    axis=1,
                )
            right = jnp.concatenate([part for _, part in quarters], axis=0)
            block = jnp.dot(left, right, preferred_element_type=jnp.float32)
            result = lax.dynamic_update_slice_in_dim(result, block, source * shard_cols, 1)
        sums.append(result)
    arrived = lax.ppermute(sums[0].astype(jnp.bfloat16), "tp", swapped("tp", 1))
    result = (sums[1] + arrived.astype(jnp.float32)).astype(jnp.bfloat16)
    return (result[None], log_part[None])


def solution(mesh):
    in_specs = (
        P("fs", ("sp", "tp"), None),
        P(),
        P("sp", "tp"),
        P("sp", "tp"),
        P("sp", "tp"),
        P("sp", "tp"),
        P(),
        P(),
        P(),
        P("tp", "sp"),
        P("tp", "sp"),
    )
    out_specs = (P("fs", ("sp", "tp"), None), P("fs", "tp", "sp"))
    return jax.shard_map(local, mesh=mesh, in_specs=in_specs, out_specs=out_specs, check_vma=False)
```

```python
import jax
import jax.numpy as jnp
from jax import lax
from jax.sharding import PartitionSpec as P

HEAD_SIZE = 64
WINDOW = 128
POOL_CH = 256


EPSILON = 1e-06
POOL_SPANS = (2, 4, 8, 16)


def passed_along(shard, axis, by):
    size = lax.axis_size(axis)
    pairs = [(i, i + by) for i in range(size) if 0 <= i + by < size]
    return lax.ppermute(shard, axis, pairs)


def windowed_attend(
    query_rows, key_rows, value_rows, key_tail, value_tail, sinks, kv_heads, group, first_pos
):
    rows = query_rows.shape[0]
    blocks = rows // WINDOW
    width = key_rows.shape[1]
    ext_keys = jnp.concatenate([key_tail, key_rows], 0)
    ext_values = jnp.concatenate([value_tail, value_rows], 0)

    def banded(table):
        return jnp.concatenate(
            [
                table[:rows].reshape(blocks, WINDOW, width),
                table[WINDOW:].reshape(blocks, WINDOW, width),
            ],
            axis=1,
        )

    band_keys = banded(ext_keys).reshape(blocks, 2 * WINDOW, kv_heads, HEAD_SIZE)
    band_values = banded(ext_values).reshape(blocks, 2 * WINDOW, kv_heads, HEAD_SIZE)
    query_blocks = query_rows.reshape(blocks, WINDOW, kv_heads, group, HEAD_SIZE)
    scores = jnp.einsum(
        "bqkgd,bskd->bkgqs", query_blocks, band_keys, preferred_element_type=jnp.float32
    ) * HEAD_SIZE ** (-0.5)
    query_pos = first_pos + jnp.arange(rows).reshape(blocks, WINDOW, 1)
    key_pos = (
        first_pos
        - WINDOW
        + jnp.arange(blocks).reshape(blocks, 1, 1) * WINDOW
        + jnp.arange(2 * WINDOW).reshape(1, 1, 2 * WINDOW)
    )
    offset = query_pos - key_pos
    allowed = (offset >= 0) & (offset < WINDOW) & (key_pos >= 0)
    scores = jnp.where(allowed[:, None, None], scores, -jnp.inf)
    sink_grid = sinks.reshape(1, kv_heads, group, 1, 1)
    top = jnp.maximum(jnp.max(scores, axis=-1, keepdims=True), sink_grid)
    weights = jnp.exp(scores - top)
    total = jnp.sum(weights, axis=-1, keepdims=True) + jnp.exp(sink_grid - top)
    probs = (weights / total).astype(jnp.bfloat16)
    mixed = jnp.einsum(
        "bkgqs,bskd->bqkgd", probs, band_values, preferred_element_type=jnp.float32
    ).astype(jnp.bfloat16)
    row_log_weight_sum = (top + jnp.log(total))[..., 0]
    return (
        mixed.reshape(rows, kv_heads * group * HEAD_SIZE),
        row_log_weight_sum.transpose(1, 2, 0, 3).reshape(kv_heads * group, rows),
    )


def pool_branch(pool_rows, pool_tail, mixing, scales, group_start, first_pos):
    rows = pool_rows.shape[0]
    columns = pool_rows.shape[1]
    pool_reach = max(POOL_SPANS)
    extended = jnp.concatenate([pool_tail, pool_rows], 0).astype(jnp.float32)
    group_index = group_start + jnp.arange(columns) // POOL_CH
    span_table = jnp.array(POOL_SPANS, jnp.int32)
    matches = group_index[:, None] == jnp.arange(len(POOL_SPANS))[None, :]
    span_of_col = jnp.sum(jnp.where(matches, span_table[None, :], 0), axis=1)
    trailing = jnp.zeros((rows, columns), jnp.float32)
    for lag in range(pool_reach):
        trailing = trailing + jnp.where(
            lag < span_of_col[None, :], extended[pool_reach - lag : pool_reach - lag + rows], 0.0
        )
    position = first_pos + jnp.arange(rows)
    count = jnp.minimum(position[:, None] + 1, span_of_col[None, :]).astype(jnp.float32)
    centred = (trailing / count - extended[pool_reach:]).astype(jnp.bfloat16)
    grouped = centred.reshape(rows, columns // POOL_CH, POOL_CH)
    product = jnp.einsum(
        "rgc,gcd->rgd", grouped, mixing, preferred_element_type=jnp.float32
    ).reshape(rows, columns)
    return (product * scales).astype(jnp.bfloat16)


def swapped(axis, bit):
    return [(i, i ^ bit) for i in range(lax.axis_size(axis))]


def sent_along(mine):
    size = lax.axis_size("sp")
    shifts = sorted(range(1, size), key=lambda d: (min(d, size - d), d))
    return [
        (d, lax.ppermute(mine, "sp", [(i, (i + d) % size) for i in range(size)])) for d in shifts
    ]


def exchanged(along, first_bit):
    size = lax.axis_size("sp")
    here = lax.axis_index("sp")
    fs_index = lax.axis_index("fs")
    gathered = []
    for step, (d, own) in enumerate(along):
        near = lax.ppermute(own, "fs", swapped("fs", 1))
        far = lax.ppermute(own, "fs", swapped("fs", 2))
        if (step + first_bit) % 2:
            corner = lax.ppermute(near, "fs", swapped("fs", 2))
        else:
            corner = lax.ppermute(far, "fs", swapped("fs", 1))
        parts = [own, near, far, corner]
        gathered.append(((here - d) % size, [(fs_index ^ k, part) for k, part in enumerate(parts)]))
    return gathered


def quarter_of(shard):
    quarter = shard.shape[0] // lax.axis_size("fs")
    return lax.dynamic_slice_in_dim(shard, lax.axis_index("fs") * quarter, quarter, 0)


def gathered_weights(in_shards, out_shards):
    in_own = jnp.concatenate(in_shards, axis=1)
    out_own = jnp.concatenate(out_shards, axis=0)
    if lax.axis_size("fs") != 4 or lax.axis_size("sp") > 8:
        in_whole = lax.all_gather(in_own, "sp", axis=0, tiled=True)
        out_whole = lax.all_gather(out_own, "sp", axis=1, tiled=True)
        return [(0, [(0, in_whole)])], [(0, [(0, out_whole)])]
    here = lax.axis_index("sp")
    in_mine = jnp.concatenate([quarter_of(shard) for shard in in_shards], axis=1)
    in_along = sent_along(in_mine)
    out_mine, in_mine = lax.optimization_barrier((quarter_of(out_own), in_mine))
    out_along = sent_along(out_mine)
    in_gathered = exchanged(in_along, 1)
    last = in_gathered[-1][1]
    held = lax.optimization_barrier(
        (tuple(part for _, part in out_along), last[1][1], last[2][1])
    )
    last[1:3] = [(last[1][0], held[1]), (last[2][0], held[2])]
    out_gathered = exchanged([(d, part) for (d, _), part in zip(out_along, held[0])], 0)
    return [(here, [(0, in_own)])] + in_gathered, [(here, [(0, out_own)])] + out_gathered


def local(
    tokens,
    norm_gain,
    query_weight,
    key_matrix,
    value_matrix,
    pool_in_weight,
    head_sink_logit,
    pool_mix,
    pool_gain,
    attn_out_weight,
    pool_out_weight,
):
    tp_index = lax.axis_index("tp")
    sp_index = lax.axis_index("sp")
    q_cols = query_weight.shape[1]
    kv_cols = key_matrix.shape[1]
    pool_cols = pool_in_weight.shape[1]
    q_heads = q_cols // HEAD_SIZE
    kv_heads = kv_cols // HEAD_SIZE
    groups_dev = pool_cols // POOL_CH
    wide = q_cols + 2 * kv_cols + pool_cols
    in_gathered, out_gathered = gathered_weights(
        (query_weight, key_matrix, value_matrix, pool_in_weight), (attn_out_weight, pool_out_weight)
    )
    own = tokens[0].astype(jnp.float32)
    scale = lax.rsqrt(jnp.mean(own * own, axis=-1, keepdims=True) + EPSILON)
    normed_own = (own * scale * norm_gain).astype(jnp.bfloat16)
    normed_peer = lax.ppermute(normed_own, "tp", swapped("tp", 1))
    half_rows = normed_own.shape[0]
    rows = 2 * half_rows
    first = tp_index == 0
    normed = jnp.concatenate(
        [jnp.where(first, normed_own, normed_peer), jnp.where(first, normed_peer, normed_own)], 0
    )
    shard_rows = query_weight.shape[0]
    total = jnp.zeros((rows, wide), jnp.float32)
    for source, quarters in in_gathered:
        if len(quarters) == 1:
            left = lax.dynamic_slice_in_dim(
                normed, source * shard_rows, quarters[0][1].shape[0], 1
            )
        else:
            left = jnp.concatenate(
                [
                    lax.dynamic_slice_in_dim(
                        normed, source * shard_rows + member * part.shape[0], part.shape[0], 1
                    )
                    for member, part in quarters
                ],
                axis=1,
            )
        right = jnp.concatenate([part for _, part in quarters], axis=0)
        total = total + jnp.dot(left, right, preferred_element_type=jnp.float32)
    projected = total.astype(jnp.bfloat16)
    first_pos = sp_index * rows
    query_rows = projected[:, :q_cols]
    key_rows = projected[:, q_cols : q_cols + kv_cols]
    value_rows = projected[:, q_cols + kv_cols : q_cols + 2 * kv_cols]
    pool_rows = projected[:, q_cols + 2 * kv_cols :]
    pool_reach = max(POOL_SPANS)
    sinks = lax.dynamic_slice_in_dim(head_sink_logit, tp_index * q_heads, q_heads, 0)
    mixing = lax.dynamic_slice_in_dim(pool_mix, tp_index * groups_dev, groups_dev, 0)
    scales = lax.dynamic_slice_in_dim(pool_gain, tp_index * pool_cols, pool_cols, 0)
    kv_tail = projected[rows - WINDOW :, q_cols : q_cols + 2 * kv_cols]
    packed = pool_rows[rows - pool_reach :].reshape(-1, 2 * kv_cols)
    tail = passed_along(jnp.concatenate([kv_tail, packed], 0), "sp", 1)
    key_tail = tail[:WINDOW, :kv_cols]
    value_tail = tail[:WINDOW, kv_cols:]
    pool_tail = tail[WINDOW:].reshape(pool_reach, pool_cols)
    attn_part, log_part = windowed_attend(
        query_rows,
        key_rows,
        value_rows,
        key_tail,
        value_tail,
        sinks,
        kv_heads,
        q_heads // kv_heads,
        first_pos,
    )
    pool_part = pool_branch(pool_rows, pool_tail, mixing, scales, tp_index * groups_dev, first_pos)
    mixers = jnp.concatenate([attn_part, pool_part], axis=1)
    shard_cols = attn_out_weight.shape[1]
    sides = [
        lax.dynamic_slice_in_dim(mixers, side * half_rows, half_rows, 0)
        for side in (1 - tp_index, tp_index)
    ]
    sums = []
    for side in sides:
        result = jnp.zeros((half_rows, shard_cols * lax.axis_size("sp")), jnp.float32)
        for source, quarters in out_gathered:
            if len(quarters) == 1:
                left = side
            else:
                left = jnp.concatenate(
                    [
                        lax.dynamic_slice_in_dim(side, member * part.shape[0], part.shape[0], 1)
                        for member, part in quarters
                    ],
                    axis=1,
                )
            right = jnp.concatenate([part for _, part in quarters], axis=0)
            block = jnp.dot(left, right, preferred_element_type=jnp.float32)
            result = lax.dynamic_update_slice_in_dim(result, block, source * shard_cols, 1)
        sums.append(result)
    arrived = lax.ppermute(sums[0].astype(jnp.bfloat16), "tp", swapped("tp", 1))
    result = (sums[1] + arrived.astype(jnp.float32)).astype(jnp.bfloat16)
    return (result[None], log_part[None])


def solution(mesh):
    in_specs = (
        P("fs", ("sp", "tp"), None),
        P(),
        P("sp", "tp"),
        P("sp", "tp"),
        P("sp", "tp"),
        P("sp", "tp"),
        P(),
        P(),
        P(),
        P("tp", "sp"),
        P("tp", "sp"),
    )
    out_specs = (P("fs", ("sp", "tp"), None), P("fs", "tp", "sp"))
    return jax.shard_map(local, mesh=mesh, in_specs=in_specs, out_specs=out_specs, check_vma=False)
```

```python
import jax
import jax.numpy as jnp
from jax import lax
from jax.sharding import PartitionSpec as P

HEAD_SIZE = 64
WINDOW = 128
POOL_CH = 256


EPSILON = 1e-06
POOL_SPANS = (2, 4, 8, 16)


def passed_along(shard, axis, by):
    size = lax.axis_size(axis)
    pairs = [(i, i + by) for i in range(size) if 0 <= i + by < size]
    return lax.ppermute(shard, axis, pairs)


def windowed_attend(
    query_rows, key_rows, value_rows, key_tail, value_tail, sinks, kv_heads, group, first_pos
):
    rows = query_rows.shape[0]
    blocks = rows // WINDOW
    width = key_rows.shape[1]
    ext_keys = jnp.concatenate([key_tail, key_rows], 0)
    ext_values = jnp.concatenate([value_tail, value_rows], 0)

    def banded(table):
        return jnp.concatenate(
            [
                table[:rows].reshape(blocks, WINDOW, width),
                table[WINDOW:].reshape(blocks, WINDOW, width),
            ],
            axis=1,
        )

    band_keys = banded(ext_keys).reshape(blocks, 2 * WINDOW, kv_heads, HEAD_SIZE)
    band_values = banded(ext_values).reshape(blocks, 2 * WINDOW, kv_heads, HEAD_SIZE)
    query_blocks = query_rows.reshape(blocks, WINDOW, kv_heads, group, HEAD_SIZE)
    scores = jnp.einsum(
        "bqkgd,bskd->bkgqs", query_blocks, band_keys, preferred_element_type=jnp.float32
    ) * HEAD_SIZE ** (-0.5)
    query_pos = first_pos + jnp.arange(rows).reshape(blocks, WINDOW, 1)
    key_pos = (
        first_pos
        - WINDOW
        + jnp.arange(blocks).reshape(blocks, 1, 1) * WINDOW
        + jnp.arange(2 * WINDOW).reshape(1, 1, 2 * WINDOW)
    )
    offset = query_pos - key_pos
    allowed = (offset >= 0) & (offset < WINDOW) & (key_pos >= 0)
    scores = jnp.where(allowed[:, None, None], scores, -jnp.inf)
    sink_grid = sinks.reshape(1, kv_heads, group, 1, 1)
    top = jnp.maximum(jnp.max(scores, axis=-1, keepdims=True), sink_grid)
    weights = jnp.exp(scores - top)
    total = jnp.sum(weights, axis=-1, keepdims=True) + jnp.exp(sink_grid - top)
    probs = (weights / total).astype(jnp.bfloat16)
    mixed = jnp.einsum(
        "bkgqs,bskd->bqkgd", probs, band_values, preferred_element_type=jnp.float32
    ).astype(jnp.bfloat16)
    row_log_weight_sum = (top + jnp.log(total))[..., 0]
    return (
        mixed.reshape(rows, kv_heads * group * HEAD_SIZE),
        row_log_weight_sum.transpose(1, 2, 0, 3).reshape(kv_heads * group, rows),
    )


def pool_branch(pool_rows, pool_tail, mixing, scales, group_start, first_pos):
    rows = pool_rows.shape[0]
    columns = pool_rows.shape[1]
    pool_reach = max(POOL_SPANS)
    extended = jnp.concatenate([pool_tail, pool_rows], 0).astype(jnp.float32)
    group_index = group_start + jnp.arange(columns) // POOL_CH
    span_table = jnp.array(POOL_SPANS, jnp.int32)
    matches = group_index[:, None] == jnp.arange(len(POOL_SPANS))[None, :]
    span_of_col = jnp.sum(jnp.where(matches, span_table[None, :], 0), axis=1)
    trailing = jnp.zeros((rows, columns), jnp.float32)
    for lag in range(pool_reach):
        trailing = trailing + jnp.where(
            lag < span_of_col[None, :], extended[pool_reach - lag : pool_reach - lag + rows], 0.0
        )
    position = first_pos + jnp.arange(rows)
    count = jnp.minimum(position[:, None] + 1, span_of_col[None, :]).astype(jnp.float32)
    centred = (trailing / count - extended[pool_reach:]).astype(jnp.bfloat16)
    grouped = centred.reshape(rows, columns // POOL_CH, POOL_CH)
    product = jnp.einsum(
        "rgc,gcd->rgd", grouped, mixing, preferred_element_type=jnp.float32
    ).reshape(rows, columns)
    return (product * scales).astype(jnp.bfloat16)


def swapped(axis, bit):
    return [(i, i ^ bit) for i in range(lax.axis_size(axis))]


def sent_along(mine):
    size = lax.axis_size("sp")
    shifts = sorted(range(1, size), key=lambda d: (min(d, size - d), d))
    return [
        (d, lax.ppermute(mine, "sp", [(i, (i + d) % size) for i in range(size)])) for d in shifts
    ]


def exchanged(along):
    return [
        (
            d,
            [
                own,
                lax.ppermute(own, "fs", swapped("fs", 1)),
                lax.ppermute(own, "fs", swapped("fs", 2)),
            ],
        )
        for d, own in along
    ]


def cornered(pieces, first_bit):
    size = lax.axis_size("sp")
    here = lax.axis_index("sp")
    fs_index = lax.axis_index("fs")
    gathered = []
    for step, (d, parts) in enumerate(pieces):
        if (step + first_bit) % 2:
            corner = lax.ppermute(parts[1], "fs", swapped("fs", 2))
        else:
            corner = lax.ppermute(parts[2], "fs", swapped("fs", 1))
        gathered.append(
            ((here - d) % size, [(fs_index ^ k, part) for k, part in enumerate(parts + [corner])])
        )
    return gathered


def quarter_of(shard):
    quarter = shard.shape[0] // lax.axis_size("fs")
    return lax.dynamic_slice_in_dim(shard, lax.axis_index("fs") * quarter, quarter, 0)


def gathered_weights(in_shards, out_shards):
    in_own = jnp.concatenate(in_shards, axis=1)
    out_own = jnp.concatenate(out_shards, axis=0)
    if lax.axis_size("fs") != 4 or lax.axis_size("sp") > 8:
        in_whole = lax.all_gather(in_own, "sp", axis=0, tiled=True)
        out_whole = lax.all_gather(out_own, "sp", axis=1, tiled=True)
        return [(0, [(0, in_whole)])], lambda ready: (ready, [(0, [(0, out_whole)])])
    here = lax.axis_index("sp")
    in_mine = jnp.concatenate([quarter_of(shard) for shard in in_shards], axis=1)
    in_along = sent_along(in_mine)
    out_mine, first = lax.optimization_barrier((quarter_of(out_own), in_along[0][1]))
    in_along[0] = (in_along[0][0], first)
    out_along = sent_along(out_mine)
    in_pieces = exchanged(in_along)
    last = in_pieces[-1][1]
    held = lax.optimization_barrier((tuple(part for _, part in out_along), last[1], last[2]))
    last[1:] = held[1:]
    in_gathered = cornered(in_pieces, 1)
    out_pieces = exchanged([(d, part) for (d, _), part in zip(out_along, held[0])])

    def finish(ready):
        ready, tied = lax.optimization_barrier((ready, [parts for _, parts in out_pieces]))
        pieces = [(d, list(parts)) for (d, _), parts in zip(out_pieces, tied)]
        return ready, [(here, [(0, out_own)])] + cornered(pieces, 0)

    return [(here, [(0, in_own)])] + in_gathered, finish


def local(
    tokens,
    norm_gain,
    query_weight,
    key_matrix,
    value_matrix,
    pool_in_weight,
    head_sink_logit,
    pool_mix,
    pool_gain,
    attn_out_weight,
    pool_out_weight,
):
    tp_index = lax.axis_index("tp")
    sp_index = lax.axis_index("sp")
    q_cols = query_weight.shape[1]
    kv_cols = key_matrix.shape[1]
    pool_cols = pool_in_weight.shape[1]
    q_heads = q_cols // HEAD_SIZE
    kv_heads = kv_cols // HEAD_SIZE
    groups_dev = pool_cols // POOL_CH
    wide = q_cols + 2 * kv_cols + pool_cols
    in_gathered, finish = gathered_weights(
        (query_weight, key_matrix, value_matrix, pool_in_weight), (attn_out_weight, pool_out_weight)
    )
    own = tokens[0].astype(jnp.float32)
    scale = lax.rsqrt(jnp.mean(own * own, axis=-1, keepdims=True) + EPSILON)
    normed_own = (own * scale * norm_gain).astype(jnp.bfloat16)
    normed_peer = lax.ppermute(normed_own, "tp", swapped("tp", 1))
    half_rows = normed_own.shape[0]
    rows = 2 * half_rows
    first = tp_index == 0
    low = jnp.where(first, normed_own, normed_peer)
    high = jnp.where(first, normed_peer, normed_own)
    shard_rows = query_weight.shape[0]

    def projected_rows(normed):
        total = jnp.zeros((half_rows, wide), jnp.float32)
        for source, quarters in in_gathered:
            if len(quarters) == 1:
                left = lax.dynamic_slice_in_dim(
                    normed, source * shard_rows, quarters[0][1].shape[0], 1
                )
            else:
                left = jnp.concatenate(
                    [
                        lax.dynamic_slice_in_dim(
                            normed, source * shard_rows + member * part.shape[0], part.shape[0], 1
                        )
                        for member, part in quarters
                    ],
                    axis=1,
                )
            right = jnp.concatenate([part for _, part in quarters], axis=0)
            total = total + jnp.dot(left, right, preferred_element_type=jnp.float32)
        return total.astype(jnp.bfloat16)

    pool_reach = max(POOL_SPANS)
    high_rows = projected_rows(high)
    kv_tail = high_rows[half_rows - WINDOW :, q_cols : q_cols + 2 * kv_cols]
    packed = high_rows[half_rows - pool_reach :, q_cols + 2 * kv_cols :].reshape(-1, 2 * kv_cols)
    tail = passed_along(jnp.concatenate([kv_tail, packed], 0), "sp", 1)
    projected = jnp.concatenate([projected_rows(low), high_rows], axis=0)
    projected, out_gathered = finish(projected)
    first_pos = sp_index * rows
    query_rows = projected[:, :q_cols]
    key_rows = projected[:, q_cols : q_cols + kv_cols]
    value_rows = projected[:, q_cols + kv_cols : q_cols + 2 * kv_cols]
    pool_rows = projected[:, q_cols + 2 * kv_cols :]
    sinks = lax.dynamic_slice_in_dim(head_sink_logit, tp_index * q_heads, q_heads, 0)
    mixing = lax.dynamic_slice_in_dim(pool_mix, tp_index * groups_dev, groups_dev, 0)
    scales = lax.dynamic_slice_in_dim(pool_gain, tp_index * pool_cols, pool_cols, 0)
    key_tail = tail[:WINDOW, :kv_cols]
    value_tail = tail[:WINDOW, kv_cols:]
    pool_tail = tail[WINDOW:].reshape(pool_reach, pool_cols)
    attn_part, log_part = windowed_attend(
        query_rows,
        key_rows,
        value_rows,
        key_tail,
        value_tail,
        sinks,
        kv_heads,
        q_heads // kv_heads,
        first_pos,
    )
    pool_part = pool_branch(pool_rows, pool_tail, mixing, scales, tp_index * groups_dev, first_pos)
    mixers = jnp.concatenate([attn_part, pool_part], axis=1)
    shard_cols = attn_out_weight.shape[1]
    sides = [
        lax.dynamic_slice_in_dim(mixers, side * half_rows, half_rows, 0)
        for side in (1 - tp_index, tp_index)
    ]
    sums = []
    for side in sides:
        result = jnp.zeros((half_rows, shard_cols * lax.axis_size("sp")), jnp.float32)
        for source, quarters in out_gathered:
            if len(quarters) == 1:
                left = side
            else:
                left = jnp.concatenate(
                    [
                        lax.dynamic_slice_in_dim(side, member * part.shape[0], part.shape[0], 1)
                        for member, part in quarters
                    ],
                    axis=1,
                )
            right = jnp.concatenate([part for _, part in quarters], axis=0)
            block = jnp.dot(left, right, preferred_element_type=jnp.float32)
            result = lax.dynamic_update_slice_in_dim(result, block, source * shard_cols, 1)
        sums.append(result)
    arrived = lax.ppermute(sums[0].astype(jnp.bfloat16), "tp", swapped("tp", 1))
    result = (sums[1] + arrived.astype(jnp.float32)).astype(jnp.bfloat16)
    return (result[None], log_part[None])


def solution(mesh):
    in_specs = (
        P("fs", ("sp", "tp"), None),
        P(),
        P("sp", "tp"),
        P("sp", "tp"),
        P("sp", "tp"),
        P("sp", "tp"),
        P(),
        P(),
        P(),
        P("tp", "sp"),
        P("tp", "sp"),
    )
    out_specs = (P("fs", ("sp", "tp"), None), P("fs", "tp", "sp"))
    return jax.shard_map(local, mesh=mesh, in_specs=in_specs, out_specs=out_specs, check_vma=False)
```
